32 devices in a mesh: ep: 8 (over z, core), tp: 4 (over y, x).
Axes of the slice: x: 2, y: 2, z: 4, core: 2. Of those that a mesh axis runs over, the one named last changes fastest.
Arguments:
- pool_input: bfloat16 [2048, 2048], P('ep'), may hold values from -6 to 6
- pool_gain: float32 [2048], replicated, may hold values from 0.1 to 1.9
- pool_weight: bfloat16 [512, 2048], P(None, 'tp'), may hold values from -0.25 to 0.25
- pool_scale: float32 [2048], P('tp'), may hold values from 0.1 to 1.9
- moe_input: bfloat16 [1536, 2048], P('ep'), may hold values from -6 to 6
- moe_gain: float32 [2048], replicated, may hold values from 0.1 to 1.9
- routes: int32 [1536, 2], P('ep'), may hold values from 0 to 7, all different within a row; in each aligned block of 192 rows (0 to 191, 192 to 383, ...) at most 96 rows name the same one
- route_logits: float32 [1536, 2], P('ep'), may hold values from -4 to 4
- gate_weight: bfloat16 [8, 2048, 4096], P('ep', None, 'tp'), may hold values from -0.125 to 0.125
- up_weight: bfloat16 [8, 2048, 4096], P('ep', None, 'tp'), may hold values from -0.125 to 0.125
- down_weight: bfloat16 [8, 2048, 4096], P('ep', None, 'tp'), may hold values from -0.09375 to 0.09375
Outputs:
- pool_out: bfloat16 [2048, 2048], P('ep', 'tp')
- expert_out: bfloat16 [1536, 2048], P('ep', 'tp')
The draws below stay inside these ranges and needn't reach their ends.
Inputs may be any that keep to these rules, and one draw needn't show every extreme that they name: `routes`: the 2 experts of a token differ. Within the rows of one device (aligned blocks of 192 rows) no expert is named by more than 96 rows, and in every draw some expert is named by exactly 96 rows of some device.
All inputs are finite; a program needn't handle non-finite values.
Results may differ from the reference program's by a relative error of at most 0.017.
Values may be sent and summed in bfloat16 or wider, within the bound.
A program may use at most 64 MiB of HBM per device.

```python
import math
from functools import partial
import jax
import jax.numpy as jnp
import numpy as np
from jax import lax

D = 2048
GROUP_WIDTH = 512
FE = 4096
TOPK = 2
TOK_B = 192
EXPERTS = 8
CAPACITY = 96
TOKENS_A = 2048
TOKENS_B = 1536
N_EP = 8
N_TP = 4


def block_scale(rng, dims, shards, low, high):
    gain = 1.0
    for axis_at, blocks in shards:
        draws = jax.random.uniform(jax.random.fold_in(jax.random.fold_in(rng, 6), axis_at), (blocks,), jnp.float32, low / len(shards), high / len(shards))
        gain = gain * jnp.repeat(jnp.exp(draws), dims[axis_at] // blocks).reshape((-1,) + (1,) * (len(dims) - 1 - axis_at))
    return gain


def assign_block(own_key, own, number, rows, amount, top, bound, slope):
    order = jax.random.permutation(own_key, amount)
    heavy_load, usual = portions_of(amount, rows * top, bound, slope, True), portions_of(amount, rows * top, bound, slope, False)
    places = jnp.arange(amount)

    def named(lengths, turn):
        used = int((lengths > 0).sum())
        fixed = max(1, used // 4)
        passed = fixed + (places - fixed + turn * (used - fixed)) % max(1, amount - fixed)
        return jnp.zeros((amount,), jnp.int32).at[order[jnp.where(places < fixed, places, passed)]].set(jnp.asarray(lengths, jnp.int32))

    lengths = jnp.where(number % 4 == 0, named(heavy_load, number // 4), named(usual, number - number // 4 - 1))
    mixed = jax.random.permutation(jax.random.fold_in(own, 3), amount)
    source_of, receiver = mixed[0:amount // 2 * 2:2], mixed[1:amount // 2 * 2:2]
    slack = jnp.minimum(lengths[source_of] - 1, bound - lengths[receiver]) // 2
    slack = jnp.where((source_of == order[0]) | (receiver == order[0]) | (lengths[receiver] == 0), 0, jnp.maximum(slack, 0))
    passed = jax.random.randint(jax.random.fold_in(own, 4), (amount // 2,), 0, 1 << 20) % (slack + 1)
    lengths = lengths.at[source_of].add(-passed).at[receiver].add(passed)
    members = jnp.searchsorted(jnp.cumsum(lengths), jnp.arange(rows * top), side="right").astype(jnp.int32)
    listing = members.reshape(top, rows).T
    listing = listing[jax.random.permutation(jax.random.fold_in(own, 1), rows)]
    turn = jax.random.randint(jax.random.fold_in(own, 2), (rows, 1), 0, top)
    return jnp.take_along_axis(listing, (jnp.arange(top)[None, :] + turn) % top, axis=1)


def portions_of(amount, total, bound, lean, full):
    loads = [(1 << 20) // math.isqrt(grade ** lean) + 1 for grade in range(1, amount + 1)]
    largest = bound if full else min(bound, max(-(-total // amount), total * loads[0] // sum(loads)))
    least = 1 if total - largest >= amount - 1 else 0
    holding, spare = [largest] + [least] * (amount - 1), total - largest - least * (amount - 1)
    while spare > 0:
        candidates = [i for i in range(1, amount) if holding[i] < largest] or [i for i in range(1, amount) if holding[i] < bound]
        whole, remaining = sum([loads[i] for i in candidates]), spare
        for i in candidates:
            more = min(bound - holding[i], max(1, remaining * loads[i] // whole), spare)
            holding[i] = holding[i] + more
            spare = spare - more
    return np.array(holding)


def gaussian(rng, shape, scale, limit, split=(), kind=jnp.bfloat16):
    drawn = scale * jax.random.normal(rng, shape, jnp.float32)
    if split:
        drawn = drawn * block_scale(rng, shape, split, -0.22, 0.18)
    return jnp.clip(drawn, -limit, limit).astype(kind)


def setup_inputs(seed: int = 0) -> dict:
    arg_keys = jax.random.split(jax.random.key(seed), 12)
    pool_input = gaussian(arg_keys[0], (TOKENS_A, D), 1.0, 6.0, ((0, 8),))
    pool_gain = jnp.clip(1.0 + 0.18 * jax.random.normal(arg_keys[1], (D,), jnp.float32), 0.1, 1.9)
    pool_weight = gaussian(arg_keys[2], (GROUP_WIDTH, D), GROUP_WIDTH ** -0.5, 0.25, ((1, 4),))
    pool_scale = jnp.clip(1.0 + 0.18 * jax.random.normal(arg_keys[3], (D,), jnp.float32), 0.1, 1.9)
    moe_input = gaussian(arg_keys[4], (TOKENS_B, D), 1.0, 6.0, ((0, 8),))
    moe_gain = jnp.clip(1.0 + 0.18 * jax.random.normal(arg_keys[5], (D,), jnp.float32), 0.1, 1.9)
    routes_keys = jax.random.split(jax.random.fold_in(arg_keys[6], 1), TOKENS_B // TOK_B)
    routes_turns = jax.random.permutation(jax.random.fold_in(arg_keys[6], 3), TOKENS_B // TOK_B)
    routes = jax.vmap(lambda own, number: assign_block(jax.random.fold_in(arg_keys[6], 2), own, number, TOK_B, EXPERTS, TOPK, CAPACITY, 2))(routes_keys, routes_turns).reshape((TOKENS_B, TOPK))
    route_logits = gaussian(arg_keys[7], (TOKENS_B, TOPK), 1.0, 4.0, ((0, 8),), jnp.float32)
    gate_weight = gaussian(arg_keys[8], (EXPERTS, D, FE), D ** -0.5, 0.125, ((0, 8), (2, 4)))
    up_weight = gaussian(arg_keys[9], (EXPERTS, D, FE), D ** -0.5, 0.125, ((0, 8), (2, 4)))
    down_weight = gaussian(arg_keys[10], (EXPERTS, D, FE), FE ** -0.5, 0.09375, ((0, 8), (2, 4)))
    return {"pool_input": pool_input, "pool_gain": pool_gain, "pool_weight": pool_weight, "pool_scale": pool_scale, "moe_input": moe_input, "moe_gain": moe_gain, "routes": routes, "route_logits": route_logits, "gate_weight": gate_weight, "up_weight": up_weight, "down_weight": down_weight}


EPSILON = 1e-06

def rms_rows(row_block, scale_gain):
    values = row_block.astype(jnp.float32)
    scaled = values * lax.rsqrt(lax.optimization_barrier(jnp.mean(values * values, axis=-1, keepdims=True)) + EPSILON)
    return (scaled * scale_gain).astype(jnp.bfloat16)

def delayed(values, offset):
    return jnp.concatenate([jnp.zeros((offset,) + values.shape[1:], values.dtype), values[:-offset]], axis=0)

def window_sums(values):
    totals = []
    current = values
    for offset in (1, 2, 4, 8):
        current = current + delayed(current, offset)
        totals.append(current)
    return totals

def slot_tables(route_block, expert_count, capacity):
    tokens_count = route_block.shape[0]
    picks_count = route_block.shape[1]
    flat_ids = route_block.reshape(-1)
    onehot = (flat_ids[:, None] == jnp.arange(expert_count, dtype=jnp.int32)[None, :]).astype(jnp.int32)
    before = jnp.cumsum(onehot, axis=0) - onehot
    rank_in = lax.optimization_barrier(jnp.sum(before * onehot, axis=1))
    slot_ids = (flat_ids * capacity + rank_in).astype(jnp.int32)
    owners = jnp.repeat(jnp.arange(tokens_count, dtype=jnp.int32), picks_count)
    holder = jnp.full((expert_count * capacity,), tokens_count, jnp.int32).at[slot_ids].set(owners)
    return (slot_ids, holder)

def pick_rows(source, indices):
    return source[indices]

def reference(pool_input, pool_gain, pool_weight, pool_scale, moe_input, moe_gain, routes, route_logits, gate_weight, up_weight, down_weight):
    normed = rms_rows(pool_input, pool_gain)
    values = normed.astype(jnp.float32)
    sums_all = window_sums(values)
    position = jnp.arange(normed.shape[0], dtype=jnp.int32)
    pieces = []
    for group_index in range(4):
        window = 2 << group_index
        first_col = group_index * GROUP_WIDTH
        counts = jnp.minimum(position + 1, window).astype(jnp.float32)
        pooled = sums_all[group_index][:, first_col:first_col + GROUP_WIDTH] / counts[:, None]
        mixed_in = (pooled - values[:, first_col:first_col + GROUP_WIDTH]).astype(jnp.bfloat16)
        pieces.append(jnp.dot(mixed_in, pool_weight[:, first_col:first_col + GROUP_WIDTH], preferred_element_type=jnp.float32))
    pool_out = (jnp.concatenate(pieces, axis=1) * pool_scale).astype(jnp.bfloat16)
    normed_b = rms_rows(moe_input, moe_gain)
    blocks = normed_b.reshape(N_EP, TOK_B, D)
    route_blocks = routes.reshape(N_EP, TOK_B, TOPK)
    slot_ids, holder = jax.vmap(partial(slot_tables, expert_count=EXPERTS, capacity=CAPACITY))(route_blocks)
    padded = jnp.concatenate([blocks, jnp.zeros((N_EP, 1, D), jnp.bfloat16)], axis=1)
    gathered = jax.vmap(pick_rows)(padded, holder)
    per_expert = gathered.reshape(N_EP, EXPERTS, CAPACITY, D).transpose(1, 0, 2, 3).reshape(EXPERTS, N_EP * CAPACITY, D)

    def run_expert(operands):
        rows_in, gate_block, up_block, down_block = operands
        rows_wide = rows_in.astype(jnp.float32)
        gate_part = jnp.dot(rows_wide, gate_block.astype(jnp.float32), preferred_element_type=jnp.float32)
        up_part = jnp.dot(rows_wide, up_block.astype(jnp.float32), preferred_element_type=jnp.float32)
        hidden = (jax.nn.silu(gate_part) * up_part).astype(jnp.bfloat16)
        share_width = FE // N_TP
        hidden_shares = hidden.reshape(rows_in.shape[0], N_TP, share_width).astype(jnp.float32)
        down_shares = down_block.reshape(D, N_TP, share_width).astype(jnp.float32)
        partial_sums = jnp.einsum('rsf,dsf->srd', hidden_shares, down_shares).astype(jnp.bfloat16)
        return lax.optimization_barrier(jnp.sum(partial_sums.astype(jnp.float32), axis=0)).astype(jnp.bfloat16)
    outputs = lax.map(run_expert, (per_expert, gate_weight, up_weight, down_weight))
    expert_ids = route_blocks.reshape(N_EP, TOK_B * TOPK)
    rank_in = slot_ids - expert_ids * CAPACITY
    block_ids = jnp.arange(N_EP, dtype=jnp.int32)[:, None]
    global_index = (expert_ids * (N_EP * CAPACITY) + block_ids * CAPACITY + rank_in).astype(jnp.int32)
    flat_out = outputs.reshape(EXPERTS * N_EP * CAPACITY, D)[global_index.reshape(-1)]
    picked = flat_out.reshape(N_EP * TOK_B, TOPK, D).astype(jnp.float32)
    raised = jnp.exp(route_logits)
    weights = raised / lax.optimization_barrier(jnp.sum(raised, axis=-1, keepdims=True))
    combined = jnp.einsum('tkd,tk->td', picked, weights)
    return (pool_out, combined.astype(jnp.bfloat16))
```

```python
import functools

import jax
import jax.numpy as jnp
from jax import lax
from jax.experimental import pallas as pl
from jax.experimental.pallas import tpu as pltpu
from jax.sharding import PartitionSpec as P

GROUP_WIDTH = 512


EPSILON = 1e-06
halo_rows = 15


def passed_along(value, axis, steps):
    count = lax.axis_size(axis)
    leading, last = (max(0, -steps), min(count, count - steps))
    return lax.ppermute(value, axis, [(source, source + steps) for source in range(leading, last)])


def rms_rows(row_block, scale_gain):
    values = row_block.astype(jnp.float32)
    scaled = values * lax.rsqrt(jnp.mean(values * values, axis=-1, keepdims=True) + EPSILON)
    return (scaled * scale_gain).astype(jnp.bfloat16)


def delayed(values, offset):
    return jnp.concatenate(
        [jnp.zeros((offset,) + values.shape[1:], values.dtype), values[:-offset]], axis=0
    )


def window_sums(values):
    totals = []
    current = values
    for offset in (1, 2, 4, 8):
        current = current + delayed(current, offset)
        totals.append(current)
    return totals


def pool_half(pool_input, pool_gain, pool_weight, pool_scale):
    normed = rms_rows(pool_input, pool_gain)
    local_rows = normed.shape[0]
    column_count = pool_weight.shape[1]
    group_index = lax.axis_index("tp") * column_count // GROUP_WIDTH
    own_group = lax.dynamic_slice_in_dim(normed, group_index * GROUP_WIDTH, GROUP_WIDTH, 1)
    earlier = passed_along(own_group[local_rows - halo_rows :], "ep", 1)
    extended = jnp.concatenate([earlier, own_group], axis=0).astype(jnp.float32)
    stacked = jnp.stack(window_sums(extended))[:, halo_rows:]
    chosen = lax.dynamic_index_in_dim(stacked, group_index, 0, keepdims=False)
    position = lax.axis_index("ep") * local_rows + lax.iota(jnp.int32, local_rows)
    window = jnp.left_shift(jnp.int32(2), group_index)
    counts = jnp.minimum(position + 1, window).astype(jnp.float32)
    mixed_in = (chosen / counts[:, None] - own_group.astype(jnp.float32)).astype(jnp.bfloat16)
    product = jnp.dot(mixed_in, pool_weight, preferred_element_type=jnp.float32)
    return (product * pool_scale).astype(jnp.bfloat16)


def expert_kernel(
    sizes,
    tokens_ref,
    gain_ref,
    select_ref,
    blend_ref,
    gate_hbm,
    up_hbm,
    down_hbm,
    out_ref,
    normed,
    outgoing,
    sibling_out,
    rows_in,
    parts,
    first_in0,
    first_in1,
    half_sum0,
    half_sum1,
    second_in0,
    second_in1,
    finished,
    returned,
    gate_ref,
    up_ref,
    down_ref,
    weight_sem,
    go_send,
    go_recv,
    a0_send,
    a0_recv,
    a1_send,
    a1_recv,
    b0_send,
    b0_recv,
    b1_send,
    b1_recv,
    ra0_send,
    ra0_recv,
    ra1_send,
    ra1_recv,
    rb0_send,
    rb0_recv,
    rb1_send,
    rb1_recv,
    back_send,
    back_recv,
):
    experts, ny, nx, slots, columns = sizes
    pairs = experts // 2
    me, shard = lax.axis_index("ep"), lax.axis_index("tp")
    my_pair, my_core = me // 2, me % 2
    my_y, my_x = shard // nx, shard % nx
    bf16, f32 = jnp.bfloat16, jnp.float32
    pending = []

    def device_at(ep, y, x):
        return {"ep": ep, "tp": y * nx + x}

    def copy_to(src, dst, send, recv, target):
        return pltpu.make_async_remote_copy(
            src_ref=src,
            dst_ref=dst,
            send_sem=send,
            recv_sem=recv,
            device_id=target,
            device_id_type=pl.DeviceIdType.MESH,
        )

    def start(*arguments):
        copy = copy_to(*arguments)
        copy.start()
        pending.append(copy)

    def arrive(ref, send, recv):
        copy_to(ref, ref, send, recv, device_at(me, my_y, my_x)).wait_recv()

    weight_copies = [
        pltpu.make_async_copy(source.at[0], target, weight_sem.at[number])
        for number, (source, target) in enumerate(
            ((gate_hbm, gate_ref), (up_hbm, up_ref), (down_hbm, down_ref))
        )
    ]
    for copy in weight_copies:
        copy.start()

    others_x = [lax.rem(my_x + step, nx) for step in range(1, nx)]
    others_y = [lax.rem(my_y + step, ny) for step in range(1, ny)]
    barrier = pltpu.get_barrier_semaphore()
    greeted = [device_at(lax.rem(me + step, experts), my_y, my_x) for step in range(1, experts)]
    greeted += [device_at(me, my_y, x) for x in others_x]
    greeted += [device_at(me, y, my_x) for y in others_y]
    for target in greeted:
        pl.semaphore_signal(
            barrier, inc=1, device_id=target, device_id_type=pl.DeviceIdType.MESH
        )

    values = tokens_ref[...].astype(f32)
    scale = lax.rsqrt(jnp.mean(values * values, axis=-1, keepdims=True) + EPSILON)
    normed[...] = (values * scale * gain_ref[...]).astype(bf16)
    own_columns = pl.ds(pl.multiple_of(shard * columns, columns), columns)
    narrow = normed[:, own_columns]

    def pair_at(step):
        return lax.rem(my_pair + step, pairs)

    for step in range(1, pairs):
        target_pair = lax.rem(my_pair + pairs - step, pairs)
        for core in range(2):
            expert = target_pair * 2 + core
            outgoing[expert] = jnp.dot(
                select_ref[expert], narrow, preferred_element_type=f32
            ).astype(bf16)
    sibling = my_pair * 2 + 1 - my_core
    wide = normed[...]
    for_sibling = jnp.dot(select_ref[sibling], wide, preferred_element_type=f32).astype(bf16)
    for_self = jnp.dot(select_ref[me], wide, preferred_element_type=f32).astype(bf16)
    my_rows = pl.ds(pl.multiple_of(my_core * slots, slots), slots)
    for y in range(ny):
        for x in range(nx):
            begin = (y * nx + x) * columns
            sibling_out[y, x] = for_sibling[:, begin : begin + columns]
            rows_in[my_pair, y, x, my_rows, :] = for_self[:, begin : begin + columns]
    pl.semaphore_wait(barrier, len(greeted))

    start(
        sibling_out,
        rows_in.at[my_pair, :, :, my_rows],
        go_send.at[sibling],
        go_recv.at[me],
        device_at(sibling, my_y, my_x),
    )
    for step in range(1, pairs):
        target_pair = lax.rem(my_pair + pairs - step, pairs)
        for core in range(2):
            expert = target_pair * 2 + core
            start(
                outgoing.at[expert],
                rows_in.at[my_pair, my_y, my_x, my_rows],
                go_send.at[expert],
                go_recv.at[me],
                device_at(expert, my_y, my_x),
            )

    def rows_of(core):
        return pl.ds(core * slots, slots)

    def spread_first(step):
        pair = pair_at(step)
        for core in range(2):
            block = rows_in.at[pair, my_y, my_x, rows_of(core)]
            source = pair * 2 + core
            arrive(block, go_send.at[source], go_recv.at[source])
            if core == 0:
                for x in others_x:
                    start(block, block, a0_send.at[pair, x], a0_recv.at[pair, my_x], device_at(me, my_y, x))
            else:
                for y in others_y:
                    start(block, block, a1_send.at[pair, y], a1_recv.at[pair, my_y], device_at(me, y, my_x))

    def spread_second(step):
        pair = pair_at(step)
        for x in others_x:
            arrive(rows_in.at[pair, my_y, x, rows_of(0)], a0_send.at[pair, x], a0_recv.at[pair, x])
        held = rows_in.at[pair, my_y, :, rows_of(0)]
        for y in others_y:
            start(held, held, b0_send.at[pair, y], b0_recv.at[pair, my_y], device_at(me, y, my_x))
        for y in others_y:
            arrive(rows_in.at[pair, y, my_x, rows_of(1)], a1_send.at[pair, y], a1_recv.at[pair, y])
        held = rows_in.at[pair, :, my_x, rows_of(1)]
        for x in others_x:
            start(held, held, b1_send.at[pair, x], b1_recv.at[pair, my_x], device_at(me, my_y, x))

    def spread_end(step):
        pair = pair_at(step)
        for y in others_y:
            arrive(rows_in.at[pair, y, :, rows_of(0)], b0_send.at[pair, y], b0_recv.at[pair, y])
        for x in others_x:
            arrive(rows_in.at[pair, :, x, rows_of(1)], b1_send.at[pair, x], b1_recv.at[pair, x])

    def multiply(step):
        pair = pair_at(step)
        entire = jnp.concatenate(
            [rows_in[pair, y, x] for y in range(ny) for x in range(nx)], axis=1
        )
        gate_part = jnp.dot(entire, gate_ref[...], preferred_element_type=f32)
        up_part = jnp.dot(entire, up_ref[...], preferred_element_type=f32)
        hidden = (gate_part / (1.0 + jnp.exp(-gate_part)) * up_part).astype(bf16)
        for y in range(ny):
            for x in range(nx):
                begin = (y * nx + x) * columns
                parts[pair, y, x] = lax.dot_general(
                    hidden,
                    down_ref[begin : begin + columns, :],
                    (((1,), (1,)), ((), ())),
                    preferred_element_type=f32,
                ).astype(bf16)
        for x in others_x:
            start(
                parts.at[pair, :, x, rows_of(0)],
                first_in0.at[pair, my_x],
                ra0_send.at[pair, x],
                ra0_recv.at[pair, my_x],
                device_at(me, my_y, x),
            )
        for y in others_y:
            start(
                parts.at[pair, y, :, rows_of(1)],
                first_in1.at[pair, my_y],
                ra1_send.at[pair, y],
                ra1_recv.at[pair, my_y],
                device_at(me, y, my_x),
            )

    def reduce_first(step):
        pair = pair_at(step)
        for x in others_x:
            arrive(first_in0.at[pair, x], ra0_send.at[pair, x], ra0_recv.at[pair, x])
        for y in range(ny):
            total = parts[pair, y, my_x, rows_of(0), :].astype(f32)
            for x in others_x:
                total += first_in0[pair, x, y].astype(f32)
            half_sum0[pair, y] = total.astype(bf16)
        for y in others_y:
            start(
                half_sum0.at[pair, y],
                second_in0.at[pair, my_y],
                rb0_send.at[pair, y],
                rb0_recv.at[pair, my_y],
                device_at(me, y, my_x),
            )
        for y in others_y:
            arrive(first_in1.at[pair, y], ra1_send.at[pair, y], ra1_recv.at[pair, y])
        for x in range(nx):
            total = parts[pair, my_y, x, rows_of(1), :].astype(f32)
            for y in others_y:
                total += first_in1[pair, y, x].astype(f32)
            half_sum1[pair, x] = total.astype(bf16)
        for x in others_x:
            start(
                half_sum1.at[pair, x],
                second_in1.at[pair, my_x],
                rb1_send.at[pair, x],
                rb1_recv.at[pair, my_x],
                device_at(me, my_y, x),
            )

    def reduce_second(step):
        pair = pair_at(step)
        for y in others_y:
            arrive(second_in0.at[pair, y], rb0_send.at[pair, y], rb0_recv.at[pair, y])
        total = half_sum0[pair, my_y].astype(f32)
        for y in others_y:
            total += second_in0[pair, y].astype(f32)
        finished[pair * 2] = total.astype(bf16)
        for x in others_x:
            arrive(second_in1.at[pair, x], rb1_send.at[pair, x], rb1_recv.at[pair, x])
        total = half_sum1[pair, my_x].astype(f32)
        for x in others_x:
            total += second_in1[pair, x].astype(f32)
        finished[pair * 2 + 1] = total.astype(bf16)
        if step == 0:
            targets = [sibling]
            returned[me] = finished[me]
        else:
            targets = [pair * 2, pair * 2 + 1]
        for target in targets:
            start(
                finished.at[target],
                returned.at[me],
                back_send.at[target],
                back_recv.at[me],
                device_at(target, my_y, my_x),
            )

    arrive(
        rows_in.at[my_pair, :, :, pl.ds(pl.multiple_of((1 - my_core) * slots, slots), slots)],
        go_send.at[sibling],
        go_recv.at[sibling],
    )
    for copy in weight_copies:
        copy.wait()
    multiply(0)
    for turn in range(1, pairs + 4):
        if turn < pairs:
            spread_first(turn)
        if 1 <= turn - 1 < pairs:
            spread_second(turn - 1)
        if 1 <= turn - 2 < pairs:
            spread_end(turn - 2)
            multiply(turn - 2)
        if 0 <= turn - 3 < pairs:
            reduce_first(turn - 3)
        if 0 <= turn - 4 < pairs:
            reduce_second(turn - 4)
    total = jnp.dot(blend_ref[me], returned[me], preferred_element_type=f32)
    for step in range(1, experts):
        source = lax.rem(me + step, experts)
        arrive(returned.at[source], back_send.at[source], back_recv.at[source])
        total += jnp.dot(blend_ref[source], returned[source], preferred_element_type=f32)
    out_ref[...] = total.astype(bf16)
    for copy in pending:
        copy.wait_send()


def expert_half(moe_input, moe_gain, routes, route_logits, gate_weight, up_weight, down_weight):
    local_rows, row_width = moe_input.shape
    picks_count = routes.shape[1]
    experts, shards = lax.axis_size("ep"), lax.axis_size("tp")
    capacity = 2 * local_rows * picks_count // experts
    slots = -(-capacity // 16) * 16
    columns = row_width // shards
    ny = max(d for d in range(1, shards + 1) if shards % d == 0 and d * d <= shards)
    nx = shards // ny
    pairs = experts // 2
    hidden_units = gate_weight.shape[2]

    expert_ids = jnp.arange(experts, dtype=jnp.int32)
    named = (routes[:, :, None] == expert_ids).astype(jnp.float32)
    visits = jnp.sum(named, axis=1)
    order = jnp.arange(local_rows, dtype=jnp.int32)
    earlier = (order[:, None] > order[None, :]).astype(jnp.float32)
    rank = jnp.dot(earlier, visits, preferred_element_type=jnp.float32).astype(jnp.int32)
    raised = jnp.exp(route_logits)
    shares = raised / jnp.sum(raised, axis=-1, keepdims=True)
    share_of = jnp.sum(named * shares[:, :, None], axis=1)
    slot_ids = jnp.arange(slots, dtype=jnp.int32)
    rank_of, visits_of = rank.T, visits.T
    select = jnp.where(
        rank_of[:, None, :] == slot_ids[None, :, None], visits_of[:, None, :], 0.0
    ).astype(jnp.bfloat16)
    blend = jnp.where(
        rank_of[:, :, None] == slot_ids[None, None, :], share_of.T[:, :, None], 0.0
    ).astype(jnp.bfloat16)

    bf16 = jnp.bfloat16
    dma = pltpu.SemaphoreType.DMA
    vmem = pl.BlockSpec(memory_space=pltpu.VMEM)
    anywhere = pl.BlockSpec(memory_space=pl.ANY)
    block = (slots, columns)
    sems_x, sems_y = dma((pairs, nx)), dma((pairs, ny))
    return pl.pallas_call(
        functools.partial(expert_kernel, (experts, ny, nx, slots, columns)),
        out_shape=jax.ShapeDtypeStruct((local_rows, columns), bf16),
        in_specs=[vmem] * 4 + [anywhere] * 3,
        out_specs=vmem,
        scratch_shapes=[
            pltpu.VMEM((local_rows, row_width), bf16),
            pltpu.VMEM((experts,) + block, bf16),
            pltpu.VMEM((ny, nx) + block, bf16),
            pltpu.VMEM((pairs, ny, nx, 2 * slots, columns), bf16),
            pltpu.VMEM((pairs, ny, nx, 2 * slots, columns), bf16),
            pltpu.VMEM((pairs, nx, ny) + block, bf16),
            pltpu.VMEM((pairs, ny, nx) + block, bf16),
            pltpu.VMEM((pairs, ny) + block, bf16),
            pltpu.VMEM((pairs, nx) + block, bf16),
            pltpu.VMEM((pairs, ny) + block, bf16),
            pltpu.VMEM((pairs, nx) + block, bf16),
            pltpu.VMEM((experts,) + block, bf16),
            pltpu.VMEM((experts,) + block, bf16),
            pltpu.VMEM((row_width, hidden_units), bf16),
            pltpu.VMEM((row_width, hidden_units), bf16),
            pltpu.VMEM((row_width, hidden_units), bf16),
            dma((3,)),
            dma((experts,)),
            dma((experts,)),
        ]
        + [sems_x, sems_x, sems_y, sems_y, sems_y, sems_y, sems_x, sems_x] * 2
        + [dma((experts,)), dma((experts,))],
        compiler_params=pltpu.CompilerParams(
            collective_id=0, has_side_effects=True, vmem_limit_bytes=58 * 1024 * 1024
        ),
    )(
        moe_input,
        moe_gain.reshape(1, row_width),
        select,
        blend,
        gate_weight,
        up_weight,
        down_weight,
    )


def local(
    pool_input,
    pool_gain,
    pool_weight,
    pool_scale,
    moe_input,
    moe_gain,
    routes,
    route_logits,
    gate_weight,
    up_weight,
    down_weight,
):
    pool_out = pool_half(pool_input, pool_gain, pool_weight, pool_scale)
    expert_out = expert_half(
        moe_input, moe_gain, routes, route_logits, gate_weight, up_weight, down_weight
    )
    return (pool_out, expert_out)


def solution(mesh):
    in_specs = (
        P("ep", None),
        P(),
        P(None, "tp"),
        P("tp"),
        P("ep", None),
        P(),
        P("ep", None),
        P("ep", None),
        P("ep", None, "tp"),
        P("ep", None, "tp"),
        P("ep", None, "tp"),
    )
    out_specs = (P("ep", "tp"), P("ep", "tp"))
    return jax.shard_map(local, mesh=mesh, in_specs=in_specs, out_specs=out_specs, check_vma=False)
```

```python
import functools

import jax
import jax.numpy as jnp
from jax import lax
from jax.experimental import pallas as pl
from jax.experimental.pallas import tpu as pltpu
from jax.sharding import PartitionSpec as P

EPSILON = 1e-06
halo_rows = 16


def expert_kernel(
    sizes,
    tokens_ref,
    gain_ref,
    select_ref,
    blend_ref,
    gate_hbm,
    up_hbm,
    down_hbm,
    pool_in_ref,
    pool_gain_ref,
    pool_weight_ref,
    pool_scale_ref,
    out_ref,
    pool_out_ref,
    normed,
    outgoing,
    sibling_out,
    rows_in,
    parts,
    first_in0,
    first_in1,
    half_sum0,
    half_sum1,
    second_in0,
    second_in1,
    finished,
    returned,
    gate_ref,
    up_ref,
    down_ref,
    pool_own,
    pool_tail,
    pool_halo,
    weight_sem,
    halo_sem,
    go_send,
    go_recv,
    a0_send,
    a0_recv,
    a1_send,
    a1_recv,
    b0_send,
    b0_recv,
    b1_send,
    b1_recv,
    ra0_send,
    ra0_recv,
    ra1_send,
    ra1_recv,
    rb0_send,
    rb0_recv,
    rb1_send,
    rb1_recv,
    back_send,
    back_recv,
):
    experts, ny, nx, slots, columns = sizes
    pairs = experts // 2
    me, shard = lax.axis_index("ep"), lax.axis_index("tp")
    my_pair, my_core = me // 2, me % 2
    my_y, my_x = shard // nx, shard % nx
    bf16, f32 = jnp.bfloat16, jnp.float32
    pending = []

    def device_at(ep, y, x):
        return {"ep": ep, "tp": y * nx + x}

    def copy_to(src, dst, send, recv, target):
        return pltpu.make_async_remote_copy(
            src_ref=src,
            dst_ref=dst,
            send_sem=send,
            recv_sem=recv,
            device_id=target,
            device_id_type=pl.DeviceIdType.MESH,
        )

    def start(*arguments):
        copy = copy_to(*arguments)
        copy.start()
        pending.append(copy)

    def arrive(ref, send, recv):
        copy_to(ref, ref, send, recv, device_at(me, my_y, my_x)).wait_recv()

    weight_copies = [
        pltpu.make_async_copy(source.at[0], target, weight_sem.at[number])
        for number, (source, target) in enumerate(
            ((gate_hbm, gate_ref), (up_hbm, up_ref), (down_hbm, down_ref))
        )
    ]
    for copy in weight_copies:
        copy.start()

    others_x = [lax.rem(my_x + step, nx) for step in range(1, nx)]
    others_y = [lax.rem(my_y + step, ny) for step in range(1, ny)]
    barrier = pltpu.get_barrier_semaphore()
    greeted = [device_at(lax.rem(me + step, experts), my_y, my_x) for step in range(1, experts)]
    greeted += [device_at(me, my_y, x) for x in others_x]
    greeted += [device_at(me, y, my_x) for y in others_y]
    for target in greeted:
        pl.semaphore_signal(
            barrier, inc=1, device_id=target, device_id_type=pl.DeviceIdType.MESH
        )

    values = tokens_ref[...].astype(f32)
    scale = lax.rsqrt(jnp.mean(values * values, axis=-1, keepdims=True) + EPSILON)
    normed[...] = (values * scale * gain_ref[...]).astype(bf16)
    own_columns = pl.ds(pl.multiple_of(shard * columns, columns), columns)
    narrow = normed[:, own_columns]

    def pair_at(step):
        if pairs > 0:
            return lax.rem(my_pair + step, pairs)
        flipped, bit = 0, 1
        while bit < pairs:
            digit = (my_pair // bit) % 2
            flipped = flipped + bit * (1 - digit if step & bit else digit)
            bit *= 2
        return flipped

    def target_at(step):
        if pairs > 0:
            return lax.rem(my_pair + pairs - step, pairs)
        return pair_at(step)

    for step in range(1, pairs):
        target_pair = target_at(step)
        for core in range(2):
            expert = target_pair * 2 + core
            outgoing[expert] = jnp.dot(
                select_ref[expert], narrow, preferred_element_type=f32
            ).astype(bf16)
    sibling = my_pair * 2 + 1 - my_core
    wide = normed[...]
    for_sibling = jnp.dot(select_ref[sibling], wide, preferred_element_type=f32).astype(bf16)
    for_self = jnp.dot(select_ref[me], wide, preferred_element_type=f32).astype(bf16)
    my_rows = pl.ds(pl.multiple_of(my_core * slots, slots), slots)
    for y in range(ny):
        for x in range(nx):
            begin = (y * nx + x) * columns
            sibling_out[y, x] = for_sibling[:, begin : begin + columns]
            rows_in[my_pair, y, x, my_rows, :] = for_self[:, begin : begin + columns]
    pl.semaphore_wait(barrier, len(greeted))

    start(
        sibling_out,
        rows_in.at[my_pair, :, :, my_rows],
        go_send.at[sibling],
        go_recv.at[me],
        device_at(sibling, my_y, my_x),
    )
    for step in range(1, pairs):
        target_pair = target_at(step)
        for core in range(2):
            expert = target_pair * 2 + core
            start(
                outgoing.at[expert],
                rows_in.at[my_pair, my_y, my_x, my_rows],
                go_send.at[expert],
                go_recv.at[me],
                device_at(expert, my_y, my_x),
            )

    group_width = pool_weight_ref.shape[0]
    group = shard * pool_weight_ref.shape[1] // group_width
    pool_rows = pool_in_ref.shape[0]
    halo_count = pool_tail.shape[0]

    def pool_start():
        inputs = pool_in_ref[...].astype(f32)
        spread = lax.rsqrt(jnp.mean(inputs * inputs, axis=-1, keepdims=True) + EPSILON)
        group_columns = pl.ds(pl.multiple_of(group * group_width, group_width), group_width)
        own = pool_in_ref[:, group_columns].astype(f32)
        pool_own[...] = (own * spread * pool_gain_ref[:, group_columns]).astype(bf16)
        pool_tail[...] = pool_own[pool_rows - halo_count :, :]
        start(
            pool_tail,
            pool_halo,
            halo_sem.at[0],
            halo_sem.at[1],
            device_at(lax.rem(me + 1, experts), my_y, my_x),
        )

    def pool_end():
        arrive(pool_halo, halo_sem.at[0], halo_sem.at[1])
        own = pool_own[...].astype(f32)
        halo = jnp.where(me == 0, 0.0, pool_halo[...].astype(f32))
        current = jnp.concatenate([halo, own], axis=0)
        chosen = jnp.zeros_like(current)
        for number in range(4):
            current = current + pltpu.roll(current, 1 << number, 0)
            chosen = jnp.where(group == number, current, chosen)
        window = jnp.where(group == 0, 2, jnp.where(group == 1, 4, jnp.where(group == 2, 8, 16)))
        position = me * pool_rows + lax.broadcasted_iota(jnp.int32, (pool_rows, 1), 0)
        counts = jnp.minimum(position + 1, window).astype(f32)
        mixed = (chosen[halo_count:] / counts - own).astype(bf16)
        product = jnp.dot(mixed, pool_weight_ref[...], preferred_element_type=f32)
        pool_out_ref[...] = (product * pool_scale_ref[...]).astype(bf16)

    sibling_rows = pl.ds(pl.multiple_of((1 - my_core) * slots, slots), slots)

    def rows_of(core):
        return pl.ds(core * slots, slots)

    def spread_first(step):
        pair = pair_at(step)
        for core in range(2):
            block = rows_in.at[pair, my_y, my_x, rows_of(core)]
            source = pair * 2 + core
            arrive(block, go_send.at[source], go_recv.at[source])
            if core == 0:
                for x in others_x:
                    start(block, block, a0_send.at[pair, x], a0_recv.at[pair, my_x], device_at(me, my_y, x))
            else:
                for y in others_y:
                    start(block, block, a1_send.at[pair, y], a1_recv.at[pair, my_y], device_at(me, y, my_x))

    def spread_second(step):
        pair = pair_at(step)
        for x in others_x:
            arrive(rows_in.at[pair, my_y, x, rows_of(0)], a0_send.at[pair, x], a0_recv.at[pair, x])
        held = rows_in.at[pair, my_y, :, rows_of(0)]
        for y in others_y:
            start(held, held, b0_send.at[pair, y], b0_recv.at[pair, my_y], device_at(me, y, my_x))
        for y in others_y:
            arrive(rows_in.at[pair, y, my_x, rows_of(1)], a1_send.at[pair, y], a1_recv.at[pair, y])
        held = rows_in.at[pair, :, my_x, rows_of(1)]
        for x in others_x:
            start(held, held, b1_send.at[pair, x], b1_recv.at[pair, my_x], device_at(me, my_y, x))

    def spread_end(step):
        pair = pair_at(step)
        for y in others_y:
            arrive(rows_in.at[pair, y, :, rows_of(0)], b0_send.at[pair, y], b0_recv.at[pair, y])
        for x in others_x:
            arrive(rows_in.at[pair, :, x, rows_of(1)], b1_send.at[pair, x], b1_recv.at[pair, x])

    def multiply(step):
        pair = pair_at(step)
        if step == 0:
            arrive(
                rows_in.at[my_pair, :, :, sibling_rows],
                go_send.at[sibling],
                go_recv.at[sibling],
            )
            for copy in weight_copies:
                copy.wait()
        entire = jnp.concatenate(
            [rows_in[pair, y, x] for y in range(ny) for x in range(nx)], axis=1
        )
        gate_part = jnp.dot(entire, gate_ref[...], preferred_element_type=f32)
        up_part = jnp.dot(entire, up_ref[...], preferred_element_type=f32)
        hidden = (gate_part / (1.0 + jnp.exp(-gate_part)) * up_part).astype(bf16)
        for y in range(ny):
            for x in range(nx):
                begin = (y * nx + x) * columns
                parts[pair, y, x] = lax.dot_general(
                    hidden,
                    down_ref[begin : begin + columns, :],
                    (((1,), (1,)), ((), ())),
                    preferred_element_type=f32,
                ).astype(bf16)

    def send_parts(step):
        pair = pair_at(step)
        for x in others_x:
            start(
                parts.at[pair, :, x, rows_of(0)],
                first_in0.at[pair, my_x],
                ra0_send.at[pair, x],
                ra0_recv.at[pair, my_x],
                device_at(me, my_y, x),
            )
        for y in others_y:
            start(
                parts.at[pair, y, :, rows_of(1)],
                first_in1.at[pair, my_y],
                ra1_send.at[pair, y],
                ra1_recv.at[pair, my_y],
                device_at(me, y, my_x),
            )

    def reduce_first(step):
        pair = pair_at(step)
        for x in others_x:
            arrive(first_in0.at[pair, x], ra0_send.at[pair, x], ra0_recv.at[pair, x])
        for y in range(ny):
            total = parts[pair, y, my_x, rows_of(0), :].astype(f32)
            for x in others_x:
                total += first_in0[pair, x, y].astype(f32)
            half_sum0[pair, y] = total.astype(bf16)
        for y in others_y:
            start(
                half_sum0.at[pair, y],
                second_in0.at[pair, my_y],
                rb0_send.at[pair, y],
                rb0_recv.at[pair, my_y],
                device_at(me, y, my_x),
            )
        for y in others_y:
            arrive(first_in1.at[pair, y], ra1_send.at[pair, y], ra1_recv.at[pair, y])
        for x in range(nx):
            total = parts[pair, my_y, x, rows_of(1), :].astype(f32)
            for y in others_y:
                total += first_in1[pair, y, x].astype(f32)
            half_sum1[pair, x] = total.astype(bf16)
        for x in others_x:
            start(
                half_sum1.at[pair, x],
                second_in1.at[pair, my_x],
                rb1_send.at[pair, x],
                rb1_recv.at[pair, my_x],
                device_at(me, my_y, x),
            )

    def reduce_second(step):
        pair = pair_at(step)
        for y in others_y:
            arrive(second_in0.at[pair, y], rb0_send.at[pair, y], rb0_recv.at[pair, y])
        total = half_sum0[pair, my_y].astype(f32)
        for y in others_y:
            total += second_in0[pair, y].astype(f32)
        finished[pair * 2] = total.astype(bf16)
        for x in others_x:
            arrive(second_in1.at[pair, x], rb1_send.at[pair, x], rb1_recv.at[pair, x])
        total = half_sum1[pair, my_x].astype(f32)
        for x in others_x:
            total += second_in1[pair, x].astype(f32)
        finished[pair * 2 + 1] = total.astype(bf16)
        if step == 0:
            targets = [sibling]
            returned[me] = finished[me]
        else:
            targets = [pair * 2, pair * 2 + 1]
        for target in targets:
            start(
                finished.at[target],
                returned.at[me],
                back_send.at[target],
                back_recv.at[me],
                device_at(target, my_y, my_x),
            )

    schedule = [(multiply, (0,)), (send_parts, (0,)), (pool_start, ())]
    for turn in range(1, pairs + 4):
        if turn < pairs:
            schedule += [(spread_first, (turn,))]
        if 1 <= turn - 1 < pairs:
            schedule += [(spread_second, (turn - 1,))]
        if turn == 2:
            schedule += [(pool_end, ())]
        if 1 <= turn - 2 < pairs:
            schedule += [(spread_end, (turn - 2,)), (multiply, (turn - 2,)), (send_parts, (turn - 2,))]
        if 0 <= turn - 3 < pairs:
            schedule += [(reduce_first, (turn - 3,))]
        if 0 <= turn - 4 < pairs:
            schedule += [(reduce_second, (turn - 4,))]
    for action, arguments in schedule:
        action(*arguments)
    total = jnp.dot(blend_ref[me], returned[me], preferred_element_type=f32)
    for step in range(1, experts):
        source = lax.rem(me + step, experts)
        arrive(returned.at[source], back_send.at[source], back_recv.at[source])
        total += jnp.dot(blend_ref[source], returned[source], preferred_element_type=f32)
    out_ref[...] = total.astype(bf16)
    for copy in pending:
        copy.wait_send()


def local(
    pool_input,
    pool_gain,
    pool_weight,
    pool_scale,
    moe_input,
    moe_gain,
    routes,
    route_logits,
    gate_weight,
    up_weight,
    down_weight,
):
    local_rows, row_width = moe_input.shape
    picks_count = routes.shape[1]
    experts, shards = lax.axis_size("ep"), lax.axis_size("tp")
    capacity = 2 * local_rows * picks_count // experts
    slots = -(-capacity // 16) * 16
    columns = row_width // shards
    ny = max(d for d in range(1, shards + 1) if shards % d == 0 and d * d <= shards)
    nx = shards // ny
    pairs = experts // 2
    hidden_units = gate_weight.shape[2]

    expert_ids = jnp.arange(experts, dtype=jnp.int32)
    named = (routes[:, :, None] == expert_ids).astype(jnp.float32)
    visits = jnp.sum(named, axis=1)
    order = jnp.arange(local_rows, dtype=jnp.int32)
    earlier = (order[:, None] > order[None, :]).astype(jnp.float32)
    rank = jnp.dot(earlier, visits, preferred_element_type=jnp.float32).astype(jnp.int32)
    raised = jnp.exp(route_logits)
    shares = raised / jnp.sum(raised, axis=-1, keepdims=True)
    share_of = jnp.sum(named * shares[:, :, None], axis=1)
    slot_ids = jnp.arange(slots, dtype=jnp.int32)
    rank_of, visits_of = rank.T, visits.T
    select = jnp.where(
        rank_of[:, None, :] == slot_ids[None, :, None], visits_of[:, None, :], 0.0
    ).astype(jnp.bfloat16)
    blend = jnp.where(
        rank_of[:, :, None] == slot_ids[None, None, :], share_of.T[:, :, None], 0.0
    ).astype(jnp.bfloat16)

    bf16 = jnp.bfloat16
    dma = pltpu.SemaphoreType.DMA
    vmem = pl.BlockSpec(memory_space=pltpu.VMEM)
    anywhere = pl.BlockSpec(memory_space=pl.ANY)
    block = (slots, columns)
    sems_x, sems_y = dma((pairs, nx)), dma((pairs, ny))
    expert_out, pool_out = pl.pallas_call(
        functools.partial(expert_kernel, (experts, ny, nx, slots, columns)),
        out_shape=(
            jax.ShapeDtypeStruct((local_rows, columns), bf16),
            jax.ShapeDtypeStruct((pool_input.shape[0], pool_weight.shape[1]), bf16),
        ),
        in_specs=[vmem] * 4 + [anywhere] * 3 + [vmem] * 4,
        out_specs=(vmem, vmem),
        scratch_shapes=[
            pltpu.VMEM((local_rows, row_width), bf16),
            pltpu.VMEM((experts,) + block, bf16),
            pltpu.VMEM((ny, nx) + block, bf16),
            pltpu.VMEM((pairs, ny, nx, 2 * slots, columns), bf16),
            pltpu.VMEM((pairs, ny, nx, 2 * slots, columns), bf16),
            pltpu.VMEM((pairs, nx, ny) + block, bf16),
            pltpu.VMEM((pairs, ny, nx) + block, bf16),
            pltpu.VMEM((pairs, ny) + block, bf16),
            pltpu.VMEM((pairs, nx) + block, bf16),
            pltpu.VMEM((pairs, ny) + block, bf16),
            pltpu.VMEM((pairs, nx) + block, bf16),
            pltpu.VMEM((experts,) + block, bf16),
            pltpu.VMEM((experts,) + block, bf16),
            pltpu.VMEM((row_width, hidden_units), bf16),
            pltpu.VMEM((row_width, hidden_units), bf16),
            pltpu.VMEM((row_width, hidden_units), bf16),
            pltpu.VMEM((pool_input.shape[0], pool_weight.shape[0]), bf16),
            pltpu.VMEM((halo_rows, pool_weight.shape[0]), bf16),
            pltpu.VMEM((halo_rows, pool_weight.shape[0]), bf16),
            dma((3,)),
            dma((2,)),
            dma((experts,)),
            dma((experts,)),
        ]
        + [sems_x, sems_x, sems_y, sems_y, sems_y, sems_y, sems_x, sems_x] * 2
        + [dma((experts,)), dma((experts,))],
        compiler_params=pltpu.CompilerParams(
            collective_id=0, has_side_effects=True, vmem_limit_bytes=58 * 1024 * 1024
        ),
    )(
        moe_input,
        moe_gain.reshape(1, row_width),
        select,
        blend,
        gate_weight,
        up_weight,
        down_weight,
        pool_input,
        pool_gain.reshape(1, row_width),
        pool_weight,
        pool_scale.reshape(1, -1),
    )
    return (pool_out, expert_out)


def solution(mesh):
    in_specs = (
        P("ep", None),
        P(),
        P(None, "tp"),
        P("tp"),
        P("ep", None),
        P(),
        P("ep", None),
        P("ep", None),
        P("ep", None, "tp"),
        P("ep", None, "tp"),
        P("ep", None, "tp"),
    )
    out_specs = (P("ep", "tp"), P("ep", "tp"))
    return jax.shard_map(local, mesh=mesh, in_specs=in_specs, out_specs=out_specs, check_vma=False)
```
